32 devices in a mesh: ep: 8 (over z, y), tp: 4 (over x, core).
Axes of the slice: x: 2, y: 2, z: 4, core: 2. Of those that a mesh axis runs over, the one named last changes fastest.
Arguments:
- hidden_in: bfloat16 [384, 2048], P('ep'), may hold values from -6 to 6
- carried_state: float32 [384, 4, 128, 256], P('ep', 'tp'), may hold values from -6 to 6
- input_gain: bfloat16 [2048], replicated, may hold values from 0.099609375 to 1.8984375
- query_weight: bfloat16 [2048, 512], P(None, 'tp'), may hold values from -0.125 to 0.125
- key_weight: bfloat16 [2048, 512], P(None, 'tp'), may hold values from -0.125 to 0.125
- value_weight: bfloat16 [2048, 1024], P(None, 'tp'), may hold values from -0.125 to 0.125
- outgate_weight: bfloat16 [2048, 1024], P(None, 'tp'), may hold values from -0.125 to 0.125
- decay_weight: bfloat16 [2048, 512], P(None, 'tp'), may hold values from -0.5 to 0.5
- decay_shift: float32 [384, 512], P('ep', 'tp'), may hold values from -0.7 to 0
- head_gain: bfloat16 [4, 256], P('tp'), may hold values from 0.099609375 to 1.8984375
- output_weight: bfloat16 [1024, 2048], P('tp'), may hold values from -0.1875 to 0.1875
- channel_gain: bfloat16 [2048], replicated, may hold values from 0.099609375 to 1.8984375
- branch_gate: bfloat16 [2048], replicated, may hold values from -0.125 to 0.125
- routes: int32 [384, 2], P('ep'), may hold values from 0 to 7, all different within a row; in each aligned block of 48 rows (0 to 47, 48 to 95, ...) at most 14 rows name the same one
- route_weights: float32 [384, 2], P('ep'), may hold values from 0.1 to 1
- expert_gate: bfloat16 [8, 2048, 3072], P('ep', None, 'tp'), may hold values from -0.125 to 0.125
- expert_up: bfloat16 [8, 2048, 3072], P('ep', None, 'tp'), may hold values from -0.125 to 0.125
- expert_down: bfloat16 [8, 3072, 2048], P('ep', 'tp'), may hold values from -0.109375 to 0.109375
- dense_gate: bfloat16 [2048, 4096], P('tp', 'ep'), may hold values from -0.125 to 0.125
- dense_up: bfloat16 [2048, 4096], P('tp', 'ep'), may hold values from -0.125 to 0.125
- dense_down: bfloat16 [4096, 2048], P('ep', 'tp'), may hold values from -0.09375 to 0.09375
Outputs:
- mixed: bfloat16 [384, 2048], P('ep', 'tp')
- new_state: float32 [384, 4, 128, 256], P('ep', 'tp')
The draws below stay inside these ranges and needn't reach their ends.
Inputs may be any that keep to these rules, and one draw needn't show every extreme that they name: `routes`: each row names 2 different experts. Among the rows of one index of ep no expert is named more than 14 times, and in every draw some expert is named exactly 14 times by the rows of some index.
All inputs are finite; a program needn't handle non-finite values.
Results may differ from the reference program's by a relative error of at most 0.02.
Values may be sent and summed in bfloat16 or wider, within the bound.
A program may use at most 128 MiB of HBM per device.

```python
import math
import jax
import jax.numpy as jnp
import numpy as np
from jax import lax

D = 2048
HEADS = 4
DK = 128
DV = 256
FF = 3072
DFF = 4096
TOPK = 2
SEQ_DEV = 48
BATCH = 384
EXPERTS = 8
CAP = 14
N_EP = 8
N_TP = 4


def level_of(stream_key, dims, pieces, smallest, largest):
    gain = 1.0
    for axis_at, blocks in pieces:
        draws = jax.random.uniform(jax.random.fold_in(jax.random.fold_in(stream_key, 6), axis_at), (blocks,), jnp.float32, smallest / len(pieces), largest / len(pieces))
        gain = gain * jnp.repeat(jnp.exp(draws), dims[axis_at] // blocks).reshape((-1,) + (1,) * (len(dims) - 1 - axis_at))
    return gain


def shared_out(key, own, number, rows, amount, top, limit, skew):
    ranking = jax.random.permutation(key, amount)
    crowded, common = shares(amount, rows * top, limit, skew, True), shares(amount, rows * top, limit, skew, False)
    places = jnp.arange(amount)

    def named(tallies, offset_by):
        used = int((tallies > 0).sum())
        fixed = max(1, used // 4)
        passed = fixed + (places - fixed + offset_by * (used - fixed)) % max(1, amount - fixed)
        return jnp.zeros((amount,), jnp.int32).at[ranking[jnp.where(places < fixed, places, passed)]].set(jnp.asarray(tallies, jnp.int32))

    tallies = jnp.where(number % 4 == 0, named(crowded, number // 4), named(common, number - number // 4 - 1))
    mixed = jax.random.permutation(jax.random.fold_in(own, 3), amount)
    donor, taker = mixed[0:amount // 2 * 2:2], mixed[1:amount // 2 * 2:2]
    slack = jnp.minimum(tallies[donor] - 1, limit - tallies[taker]) // 2
    slack = jnp.where((donor == ranking[0]) | (taker == ranking[0]) | (tallies[taker] == 0), 0, jnp.maximum(slack, 0))
    passed = jax.random.randint(jax.random.fold_in(own, 4), (amount // 2,), 0, 1 << 20) % (slack + 1)
    tallies = tallies.at[donor].add(-passed).at[taker].add(passed)
    members = jnp.searchsorted(jnp.cumsum(tallies), jnp.arange(rows * top), side="right").astype(jnp.int32)
    table = members.reshape(top, rows).T
    table = table[jax.random.permutation(jax.random.fold_in(own, 1), rows)]
    offset_by = jax.random.randint(jax.random.fold_in(own, 2), (rows, 1), 0, top)
    return jnp.take_along_axis(table, (jnp.arange(top)[None, :] + offset_by) % top, axis=1)


def shares(count, total, reach, slope, full):
    loads = [(1 << 20) // math.isqrt(standing ** slope) + 1 for standing in range(1, count + 1)]
    largest = reach if full else min(reach, max(-(-total // count), total * loads[0] // sum(loads)))
    least = 1 if total - largest >= count - 1 else 0
    counts, spare = [largest] + [least] * (count - 1), total - largest - least * (count - 1)
    while spare > 0:
        movable = [i for i in range(1, count) if counts[i] < largest] or [i for i in range(1, count) if counts[i] < reach]
        pool, remaining = sum([loads[i] for i in movable]), spare
        for i in movable:
            extra = min(reach - counts[i], max(1, remaining * loads[i] // pool), spare)
            counts[i] = counts[i] + extra
            spare = spare - extra
    return np.array(counts)


def gaussian(rng, dims, deviation, most, shards=(), held_as=jnp.bfloat16):
    values = deviation * jax.random.normal(rng, dims, jnp.float32)
    if shards:
        values = values * level_of(rng, dims, shards, -0.22, 0.18)
    return jnp.clip(values, -most, most).astype(held_as)


def setup_inputs(seed: int = 0) -> dict:
    streams_of = jax.random.split(jax.random.key(seed), 22)
    hidden_in = gaussian(streams_of[0], (BATCH, D), 1.0, 6.0, ((0, 8),))
    carried_state = gaussian(streams_of[1], (BATCH, HEADS, DK, DV), 1.0, 6.0, ((0, 8), (1, 4)), jnp.float32)
    input_gain = jnp.clip(1.0 + 0.18 * jax.random.normal(streams_of[2], (D,), jnp.float32), 0.099609375, 1.8984375).astype(jnp.bfloat16)
    query_weight = gaussian(streams_of[3], (D, HEADS * DK), D ** -0.5, 0.125, ((1, 4),))
    key_weight = gaussian(streams_of[4], (D, HEADS * DK), D ** -0.5, 0.125, ((1, 4),))
    value_weight = gaussian(streams_of[5], (D, HEADS * DV), D ** -0.5, 0.125, ((1, 4),))
    outgate_weight = gaussian(streams_of[6], (D, HEADS * DV), D ** -0.5, 0.125, ((1, 4),))
    decay_weight = gaussian(streams_of[7], (D, HEADS * DK), (D // 16) ** -0.5, 0.5, ((1, 4),))
    decay_shift = jnp.clip(-0.7 + 0.7 * jax.random.uniform(streams_of[8], (BATCH, HEADS * DK), jnp.float32) ** level_of(streams_of[8], (BATCH, HEADS * DK), ((0, 8), (1, 4)), -0.2, 0.2), -0.7, 0.0)
    head_gain = jnp.clip(1.0 + 0.18 * jax.random.normal(streams_of[9], (HEADS, DV), jnp.float32), 0.099609375, 1.8984375).astype(jnp.bfloat16)
    output_weight = gaussian(streams_of[10], (HEADS * DV, D), (HEADS * DV) ** -0.5, 0.1875, ((0, 4),))
    channel_gain = jnp.clip(1.0 + 0.18 * jax.random.normal(streams_of[11], (D,), jnp.float32), 0.099609375, 1.8984375).astype(jnp.bfloat16)
    branch_gate = gaussian(streams_of[12], (D,), D ** -0.5, 0.125)
    routes_keys = jax.random.split(jax.random.fold_in(streams_of[13], 1), BATCH // SEQ_DEV)
    routes_turns = jax.random.permutation(jax.random.fold_in(streams_of[13], 3), BATCH // SEQ_DEV)
    routes = jax.vmap(lambda own, number: shared_out(jax.random.fold_in(streams_of[13], 2), own, number, SEQ_DEV, EXPERTS, TOPK, CAP, 2))(routes_keys, routes_turns).reshape((BATCH, TOPK))
    route_weights = jnp.clip(0.1 + 0.9 * jax.random.uniform(streams_of[14], (BATCH, TOPK), jnp.float32) ** level_of(streams_of[14], (BATCH, TOPK), ((0, 8),), -0.2, 0.2), 0.1, 1.0)
    expert_gate = gaussian(streams_of[15], (EXPERTS, D, FF), D ** -0.5, 0.125, ((0, 8), (2, 4)))
    expert_up = gaussian(streams_of[16], (EXPERTS, D, FF), D ** -0.5, 0.125, ((0, 8), (2, 4)))
    expert_down = gaussian(streams_of[17], (EXPERTS, FF, D), FF ** -0.5, 0.109375, ((0, 8), (1, 4)))
    dense_gate = gaussian(streams_of[18], (D, DFF), D ** -0.5, 0.125, ((0, 4), (1, 8)))
    dense_up = gaussian(streams_of[19], (D, DFF), D ** -0.5, 0.125, ((0, 4), (1, 8)))
    dense_down = gaussian(streams_of[20], (DFF, D), DFF ** -0.5, 0.09375, ((0, 8), (1, 4)))
    return dict(hidden_in=hidden_in, carried_state=carried_state, input_gain=input_gain, query_weight=query_weight, key_weight=key_weight, value_weight=value_weight, outgate_weight=outgate_weight, decay_weight=decay_weight, decay_shift=decay_shift, head_gain=head_gain, output_weight=output_weight, channel_gain=channel_gain, branch_gate=branch_gate, routes=routes, route_weights=route_weights, expert_gate=expert_gate, expert_up=expert_up, expert_down=expert_down, dense_gate=dense_gate, dense_up=dense_up, dense_down=dense_down)


EPSILON = 1e-06
TAU_DECAY = 16.0

def rms_factor(values):
    return lax.rsqrt(lax.optimization_barrier(jnp.mean(values * values, axis=-1, keepdims=True)) + EPSILON)

def rounded(values):
    return lax.optimization_barrier(values.astype(jnp.bfloat16)).astype(jnp.float32)

def matmul(left, right):
    return jnp.dot(left, right, preferred_element_type=jnp.float32)

def expert_apply(token_rows, gate_matrix, up_matrix, down_matrix):
    block_width = gate_matrix.shape[1] // N_TP
    total = jnp.zeros((token_rows.shape[0], down_matrix.shape[1]), jnp.float32)
    for block in range(N_TP):
        lower = block * block_width
        gate_part = matmul(token_rows, gate_matrix[:, lower:lower + block_width])
        up_part = matmul(token_rows, up_matrix[:, lower:lower + block_width])
        hidden = (jax.nn.silu(gate_part) * up_part).astype(jnp.bfloat16)
        total = total + rounded(matmul(hidden, down_matrix[lower:lower + block_width]))
    return total

def reference(hidden_in, carried_state, input_gain, query_weight, key_weight, value_weight, outgate_weight, decay_weight, decay_shift, head_gain, output_weight, channel_gain, branch_gate, routes, route_weights, expert_gate, expert_up, expert_down, dense_gate, dense_up, dense_down):
    batch_size, width = hidden_in.shape
    head_count, key_dim, value_dim = carried_state.shape[1:]
    inputs = hidden_in.astype(jnp.float32)
    normed = (inputs * rms_factor(inputs) * input_gain.astype(jnp.float32)).astype(jnp.bfloat16)
    query = matmul(normed, query_weight).astype(jnp.bfloat16)
    key_rows = matmul(normed, key_weight).astype(jnp.bfloat16)
    value_rows = matmul(normed, value_weight).astype(jnp.bfloat16)
    outgate = matmul(normed, outgate_weight).astype(jnp.bfloat16)
    decay = jnp.exp(jax.nn.log_sigmoid(matmul(normed, decay_weight)) / TAU_DECAY + decay_shift)
    decay = decay.reshape(batch_size, head_count, key_dim)
    query_scaled = query.astype(jnp.float32).reshape(batch_size, head_count, key_dim) * key_dim ** (-0.5)
    key_vals = key_rows.astype(jnp.float32).reshape(batch_size, head_count, key_dim)
    value_vals = value_rows.astype(jnp.float32).reshape(batch_size, head_count, value_dim)
    new_state = decay[..., None] * carried_state + key_vals[..., None] * value_vals[:, :, None, :]
    readout = jnp.einsum('bhk,bhkv->bhv', query_scaled, new_state, precision=lax.Precision.HIGHEST)
    gate_vals = jax.nn.silu(outgate.astype(jnp.float32).reshape(batch_size, head_count, value_dim))
    gated = (readout * rms_factor(readout) * head_gain.astype(jnp.float32) * gate_vals).astype(jnp.bfloat16)
    group = head_count // N_TP
    attended = jnp.zeros((batch_size, width), jnp.float32)
    for block in range(N_TP):
        head_rows = gated[:, block * group:(block + 1) * group].reshape(batch_size, group * value_dim)
        weight_rows = output_weight[block * group * value_dim:(block + 1) * group * value_dim]
        attended = attended + rounded(matmul(head_rows, weight_rows))
    middle = rounded(inputs + attended)
    scaled = middle * rms_factor(middle) * channel_gain.astype(jnp.float32)
    branch = jax.nn.sigmoid(lax.optimization_barrier(jnp.sum(scaled * branch_gate.astype(jnp.float32), axis=-1)))
    ffn_in = scaled.astype(jnp.bfloat16)
    dense_hidden = (jax.nn.silu(matmul(ffn_in, dense_gate)) * matmul(ffn_in, dense_up)).astype(jnp.bfloat16)
    dense = matmul(dense_hidden, dense_down)
    topk = routes.shape[1]
    flat_routes = routes.reshape(-1)
    flat_tokens = (jnp.arange(flat_routes.shape[0], dtype=jnp.int32) // topk).astype(jnp.int32)
    flat_weights = route_weights.reshape(-1)
    capacity = N_EP * CAP

    def one_expert(carry, index):
        order = jnp.argsort((flat_routes != index).astype(jnp.int32), stable=True)[:capacity]
        valid = flat_routes[order] == index
        token_ids = flat_tokens[order]
        result = expert_apply(ffn_in[token_ids], expert_gate[index], expert_up[index], expert_down[index])
        weights = jnp.where(valid, flat_weights[order], jnp.zeros_like(flat_weights[order]))
        return (carry.at[token_ids].add(weights[:, None] * result), None)
    routed, _ = lax.scan(one_expert, jnp.zeros((batch_size, width), jnp.float32), jnp.arange(expert_gate.shape[0], dtype=jnp.int32))
    mixed = (middle + branch[:, None] * dense + routed).astype(jnp.bfloat16)
    return (mixed, new_state)
```

```python
import functools

import jax
import jax.numpy as jnp
from jax import lax
from jax.experimental import pallas as pl
from jax.experimental.pallas import tpu as pltpu
from jax.sharding import PartitionSpec as P

EPSILON = 1e-06
TAU_DECAY = 16.0
MESH = pl.DeviceIdType.MESH


def rms_factor(values):
    return lax.rsqrt(jnp.mean(values * values, axis=-1, keepdims=True) + EPSILON)


def matmul(left, right):
    return jnp.dot(left, right, preferred_element_type=jnp.float32)


def silu(values):
    return values * jax.nn.sigmoid(values)


def layer_kernel(
    n_ep,
    n_tp,
    gated_ref,
    outw_ref,
    hid_ref,
    gain_ref,
    gate_ref,
    sel_ref,
    comb_hi_ref,
    comb_lo_ref,
    eg_hbm,
    eu_hbm,
    ed_hbm,
    dg_hbm,
    du_hbm,
    dd_hbm,
    mixed_ref,
    eg,
    eu,
    ed,
    dgw,
    duw,
    ddw,
    sel_recv,
    p_send,
    p_recv,
    st_send,
    st_recv,
    mid_buf,
    br_buf,
    piece,
    rows_all,
    g_send,
    g_recv,
    u_send,
    u_recv,
    e_hid,
    eo_send,
    eo_recv,
    d_hid,
    out_send,
    out_recv,
    ret_send,
    ret,
    w_sem,
    tp_ssem,
    tp_rsem,
    ep_ssem,
    ep_rsem,
):
    f32, bf16 = jnp.float32, jnp.bfloat16
    ep = lax.axis_index("ep")
    tp = lax.axis_index("tp")
    tokens, quarter = hid_ref.shape
    width = quarter * n_tp
    cap = sel_ref.shape[1]

    loads = []
    for i, (src, dst) in enumerate(
        ((dg_hbm, dgw), (du_hbm, duw), (eg_hbm, eg), (eu_hbm, eu), (ed_hbm, ed), (dd_hbm, ddw))
    ):
        load = pltpu.make_async_copy(src, dst, w_sem.at[i])
        load.start()
        loads.append(load)

    barrier = pltpu.get_barrier_semaphore()
    for d in range(1, n_tp):
        pl.semaphore_signal(
            barrier, inc=1, device_id=(ep, lax.rem(tp + d, n_tp)), device_id_type=MESH
        )
    for d in range(1, n_ep):
        pl.semaphore_signal(
            barrier, inc=1, device_id=(lax.rem(ep + d, n_ep), tp), device_id_type=MESH
        )

    def over_tp(phase, src_of, dst_of):
        copies = []
        for d in range(1, n_tp):
            peer = lax.rem(tp + d, n_tp)
            copy = pltpu.make_async_remote_copy(
                src_ref=src_of(peer),
                dst_ref=dst_of(d),
                send_sem=tp_ssem.at[phase, d - 1],
                recv_sem=tp_rsem.at[phase, d - 1],
                device_id=(ep, peer),
                device_id_type=MESH,
            )
            copy.start()
            copies.append(copy)
        return copies

    def over_ep(phase, src_of, dst_of):
        copies = []
        for d in range(1, n_ep):
            peer = lax.rem(ep + d, n_ep)
            copy = pltpu.make_async_remote_copy(
                src_ref=src_of(peer),
                dst_ref=dst_of(d),
                send_sem=ep_ssem.at[phase, d - 1],
                recv_sem=ep_rsem.at[phase, d - 1],
                device_id=(peer, tp),
                device_id_type=MESH,
            )
            copy.start()
            copies.append(copy)
        return copies

    def arrive(copies):
        for copy in copies:
            copy.wait_recv()

    for j in range(n_tp):
        p_send[j] = matmul(gated_ref[...], outw_ref[:, j * quarter : (j + 1) * quarter]).astype(bf16)
    pl.semaphore_wait(barrier, n_tp + n_ep - 2)
    c_part = over_tp(0, lambda peer: p_send.at[peer], lambda d: p_recv.at[d - 1])
    c_sel = over_ep(0, lambda peer: sel_ref.at[peer], lambda d: sel_recv.at[ep])
    sel_recv[ep] = sel_ref[ep]
    attended = p_send[tp].astype(f32)
    for d in range(1, n_tp):
        c_part[d - 1].wait_recv()
        attended = attended + p_recv[d - 1].astype(f32)
    middle = (hid_ref[...].astype(f32) + attended).astype(bf16).astype(f32)
    gain = gain_ref[...]
    squares = jnp.sum(middle * middle, axis=-1, keepdims=True)
    inner = jnp.sum(middle * gain * gate_ref[...], axis=-1, keepdims=True)
    lane = lax.broadcasted_iota(jnp.int32, (tokens, 128), 1)
    st_send[...] = jnp.where(lane < 64, squares, inner)
    c_stat = over_tp(1, lambda peer: st_send, lambda d: st_recv.at[d - 1])
    mid_buf[...] = middle
    totals = st_send[...]
    for d in range(1, n_tp):
        c_stat[d - 1].wait_recv()
        totals = totals + st_recv[d - 1]
    factor = lax.rsqrt(totals[:, 0:1] / width + EPSILON)
    br_buf[...] = jnp.broadcast_to(jax.nn.sigmoid(totals[:, 64:65] * factor), (tokens, 128))
    piece[ep] = (middle * factor * gain).astype(bf16)
    c_piece = over_ep(1, lambda peer: piece.at[ep], lambda d: piece.at[ep])

    arrive(c_sel)
    for d in range(n_ep):
        if d:
            c_piece[d - 1].wait_recv()
        source = lax.rem(ep - d + n_ep, n_ep)
        picked = matmul(sel_recv[source][:, :tokens], piece[source]).astype(bf16)
        rows_all[tp, pl.ds(pl.multiple_of(source * cap, cap), cap), :] = picked
    c_rows = over_tp(2, lambda peer: rows_all.at[tp], lambda d: rows_all.at[tp])

    loads[0].wait()
    loads[1].wait()
    everyone = piece[...].reshape(n_ep * tokens, quarter)
    units = dgw.shape[1]
    share = n_ep * tokens // n_tp
    g_send[...] = matmul(everyone, dgw[...]).astype(bf16).reshape(n_tp, share, units)
    c_g = over_tp(3, lambda peer: g_send.at[peer], lambda d: g_recv.at[d - 1])
    u_send[...] = matmul(everyone, duw[...]).astype(bf16).reshape(n_tp, share, units)
    c_u = over_tp(4, lambda peer: u_send.at[peer], lambda d: u_recv.at[d - 1])

    loads[2].wait()
    loads[3].wait()
    arrive(c_rows)
    block = eg.shape[1]
    tile = 256 if block % 256 == 0 else 128

    @pl.loop(0, block // tile)
    def _(i):
        cols = pl.ds(pl.multiple_of(i * tile, tile), tile)
        gate_part = matmul(rows_all[0], eg[0:quarter, cols])
        up_part = matmul(rows_all[0], eu[0:quarter, cols])
        for j in range(1, n_tp):
            span = slice(j * quarter, (j + 1) * quarter)
            gate_part = gate_part + matmul(rows_all[j], eg[span, cols])
            up_part = up_part + matmul(rows_all[j], eu[span, cols])
        e_hid[:, cols] = (silu(gate_part) * up_part).astype(bf16)

    g_sum = g_send[tp].astype(f32)
    u_sum = u_send[tp].astype(f32)
    for d in range(1, n_tp):
        c_g[d - 1].wait_recv()
        g_sum = g_sum + g_recv[d - 1].astype(f32)
    for d in range(1, n_tp):
        c_u[d - 1].wait_recv()
        u_sum = u_sum + u_recv[d - 1].astype(f32)
    d_hid[tp] = (silu(g_sum) * u_sum).astype(bf16)
    c_hid = over_tp(5, lambda peer: d_hid.at[tp], lambda d: d_hid.at[tp])

    loads[4].wait()
    for j in range(n_tp):
        eo_send[j] = matmul(e_hid[...], ed[:, j * quarter : (j + 1) * quarter]).astype(bf16)
    c_eo = over_tp(6, lambda peer: eo_send.at[peer], lambda d: eo_recv.at[d - 1])

    loads[5].wait()
    arrive(c_hid)
    hidden = d_hid[...].reshape(n_ep * tokens, units)
    out_send[...] = matmul(hidden, ddw[...]).astype(bf16).reshape(n_ep, tokens, quarter)
    c_out = over_ep(2, lambda peer: out_send.at[peer], lambda d: out_recv.at[d - 1])

    summed = eo_send[tp].astype(f32)
    for d in range(1, n_tp):
        c_eo[d - 1].wait_recv()
        summed = summed + eo_recv[d - 1].astype(f32)
    ret_send[...] = summed.astype(bf16).reshape(n_ep, cap, quarter)
    c_ret = over_ep(3, lambda peer: ret_send.at[peer], lambda d: ret.at[ep])
    ret[ep] = ret_send[ep]

    dense = out_send[ep].astype(f32)
    for d in range(1, n_ep):
        c_out[d - 1].wait_recv()
        dense = dense + out_recv[d - 1].astype(f32)
    arrive(c_ret)
    answers = ret[...].reshape(n_ep * cap, quarter)
    routed = matmul(comb_hi_ref[...], answers) + matmul(comb_lo_ref[...], answers)
    mixed_ref[...] = (mid_buf[...] + br_buf[:, 0:1] * dense + routed).astype(bf16)

    for copies in (c_part, c_sel, c_stat, c_piece, c_rows, c_g, c_u, c_hid, c_eo, c_out, c_ret):
        for copy in copies:
            copy.wait_send()


def run_layer(gated, output_weight, hid, gain, gate, sel, comb_hi, comb_lo, eg, eu, ed, dg, du, dd):
    n_ep, n_tp = lax.axis_size("ep"), lax.axis_size("tp")
    tokens, quarter = hid.shape
    cap = sel.shape[1]
    items = n_ep * cap
    share = n_ep * tokens // n_tp
    units = dg.shape[1]
    bf16, f32 = jnp.bfloat16, jnp.float32
    vmem = pl.BlockSpec(memory_space=pltpu.VMEM)
    anyspace = pl.BlockSpec(memory_space=pl.ANY)
    scratch = [pltpu.VMEM(w.shape, bf16) for w in (eg, eu, ed, dg, du, dd)]
    scratch += [
        pltpu.VMEM(sel.shape, bf16),
        pltpu.VMEM((n_tp, tokens, quarter), bf16),
        pltpu.VMEM((n_tp - 1, tokens, quarter), bf16),
        pltpu.VMEM((tokens, 128), f32),
        pltpu.VMEM((n_tp - 1, tokens, 128), f32),
        pltpu.VMEM((tokens, quarter), f32),
        pltpu.VMEM((tokens, 128), f32),
        pltpu.VMEM((n_ep, tokens, quarter), bf16),
        pltpu.VMEM((n_tp, items, quarter), bf16),
        pltpu.VMEM((n_tp, share, units), bf16),
        pltpu.VMEM((n_tp - 1, share, units), bf16),
        pltpu.VMEM((n_tp, share, units), bf16),
        pltpu.VMEM((n_tp - 1, share, units), bf16),
        pltpu.VMEM((items, eg.shape[1]), bf16),
        pltpu.VMEM((n_tp, items, quarter), bf16),
        pltpu.VMEM((n_tp - 1, items, quarter), bf16),
        pltpu.VMEM((n_tp, share, units), bf16),
        pltpu.VMEM((n_ep, tokens, quarter), bf16),
        pltpu.VMEM((n_ep - 1, tokens, quarter), bf16),
        pltpu.VMEM((n_ep, cap, quarter), bf16),
        pltpu.VMEM((n_ep, cap, quarter), bf16),
        pltpu.SemaphoreType.DMA((6,)),
        pltpu.SemaphoreType.DMA((7, n_tp - 1)),
        pltpu.SemaphoreType.DMA((7, n_tp - 1)),
        pltpu.SemaphoreType.DMA((4, n_ep - 1)),
        pltpu.SemaphoreType.DMA((4, n_ep - 1)),
    ]
    return pl.pallas_call(
        functools.partial(layer_kernel, n_ep, n_tp),
        out_shape=jax.ShapeDtypeStruct((tokens, quarter), bf16),
        in_specs=[vmem] * 8 + [anyspace] * 6,
        out_specs=vmem,
        scratch_shapes=scratch,
        compiler_params=pltpu.CompilerParams(
            collective_id=0, has_side_effects=True, vmem_limit_bytes=60 * 1024 * 1024
        ),
    )(gated, output_weight, hid, gain, gate, sel, comb_hi, comb_lo, eg, eu, ed, dg, du, dd)


def body(
    hidden_in,
    carried_state,
    input_gain,
    query_weight,
    key_weight,
    value_weight,
    outgate_weight,
    decay_weight,
    decay_shift,
    head_gain,
    output_weight,
    channel_gain,
    branch_gate,
    routes,
    route_weights,
    expert_gate,
    expert_up,
    expert_down,
    dense_gate,
    dense_up,
    dense_down,
):
    tokens_here, width = hidden_in.shape
    heads_here, key_dim, value_dim = carried_state.shape[1:]
    quarter = width // lax.axis_size("tp")
    lane_start = lax.axis_index("tp") * quarter
    inputs = hidden_in.astype(jnp.float32)
    normed = (inputs * rms_factor(inputs) * input_gain.astype(jnp.float32)).astype(jnp.bfloat16)
    query = matmul(normed, query_weight).astype(jnp.bfloat16)
    key_rows = matmul(normed, key_weight).astype(jnp.bfloat16)
    value_rows = matmul(normed, value_weight).astype(jnp.bfloat16)
    outgate = matmul(normed, outgate_weight).astype(jnp.bfloat16)
    decay = jnp.exp(jax.nn.log_sigmoid(matmul(normed, decay_weight)) / TAU_DECAY + decay_shift)
    decay = decay.reshape(tokens_here, heads_here, key_dim)
    query_scaled = query.astype(jnp.float32).reshape(
        tokens_here, heads_here, key_dim
    ) * key_dim ** (-0.5)
    key_vals = key_rows.astype(jnp.float32).reshape(tokens_here, heads_here, key_dim)
    value_vals = value_rows.astype(jnp.float32).reshape(tokens_here, heads_here, value_dim)
    new_state = decay[..., None] * carried_state + key_vals[..., None] * value_vals[:, :, None, :]
    readout = jnp.einsum("bhk,bhkv->bhv", query_scaled, new_state, precision=lax.Precision.HIGHEST)
    gate_vals = jax.nn.silu(outgate.astype(jnp.float32).reshape(tokens_here, heads_here, value_dim))
    gated = (readout * rms_factor(readout) * head_gain.astype(jnp.float32) * gate_vals).astype(
        jnp.bfloat16
    )
    gated = gated.reshape(tokens_here, heads_here * value_dim)
    hid_own = lax.dynamic_slice_in_dim(hidden_in, lane_start, quarter, 1)
    own_gain = lax.dynamic_slice_in_dim(channel_gain, lane_start, quarter, 0)
    own_branch = lax.dynamic_slice_in_dim(branch_gate, lane_start, quarter, 0)
    expert_count = lax.axis_size("ep")
    topk = routes.shape[1]
    capacity = tokens_here * topk // expert_count + 2
    cap = (capacity + 15) // 16 * 16
    chosen = (
        routes[:, :, None] == jnp.arange(expert_count, dtype=jnp.int32)[None, None, :]
    ).astype(jnp.int32)
    chosen_flat = chosen.reshape(tokens_here * topk, expert_count)
    index = jnp.arange(tokens_here * topk, dtype=jnp.int32)
    before = (index[:, None] > index[None, :]).astype(jnp.bfloat16)
    earlier = matmul(before, chosen_flat.astype(jnp.bfloat16))
    slot_index = jnp.sum(earlier * chosen_flat, axis=1).astype(jnp.int32)
    position = routes * cap + slot_index.reshape(tokens_here, topk)
    slot_table = jnp.arange(expert_count * cap, dtype=jnp.int32)
    sel = jnp.sum((slot_table[:, None, None] == position[None, :, :]).astype(jnp.float32), axis=2)
    sel = jnp.pad(sel, ((0, 0), (0, -tokens_here % 128))).astype(jnp.bfloat16)
    sel = sel.reshape(expert_count, cap, sel.shape[1])
    comb = jnp.sum(
        jnp.where(position[:, :, None] == slot_table, route_weights[:, :, None], 0.0), axis=1
    )
    comb_hi = lax.optimization_barrier(comb.astype(jnp.bfloat16))
    comb_lo = (comb - comb_hi.astype(jnp.float32)).astype(jnp.bfloat16)
    mixed = run_layer(
        gated,
        output_weight,
        hid_own,
        own_gain.astype(jnp.float32)[None, :],
        own_branch.astype(jnp.float32)[None, :],
        sel,
        comb_hi,
        comb_lo,
        expert_gate[0],
        expert_up[0],
        expert_down[0],
        dense_gate,
        dense_up,
        dense_down,
    )
    return (mixed, new_state)


def solution(mesh):
    in_specs = (
        P("ep", None),
        P("ep", "tp", None, None),
        P(),
        P(None, "tp"),
        P(None, "tp"),
        P(None, "tp"),
        P(None, "tp"),
        P(None, "tp"),
        P("ep", "tp"),
        P("tp", None),
        P("tp", None),
        P(),
        P(),
        P("ep", None),
        P("ep", None),
        P("ep", None, "tp"),
        P("ep", None, "tp"),
        P("ep", "tp", None),
        P("tp", "ep"),
        P("tp", "ep"),
        P("ep", "tp"),
    )
    out_specs = (P("ep", "tp"), P("ep", "tp", None, None))
    return jax.shard_map(body, mesh=mesh, in_specs=in_specs, out_specs=out_specs, check_vma=False)
```

```python
import functools

import jax
import jax.numpy as jnp
from jax import lax
from jax.experimental import pallas as pl
from jax.experimental.pallas import tpu as pltpu
from jax.sharding import PartitionSpec as P

EPSILON = 1e-06
TAU_DECAY = 16.0
MESH = pl.DeviceIdType.MESH


def rms_factor(values):
    return lax.rsqrt(jnp.mean(values * values, axis=-1, keepdims=True) + EPSILON)


def matmul(left, right):
    return jnp.dot(left, right, preferred_element_type=jnp.float32)


def silu(values):
    return values * jax.nn.sigmoid(values)


def layer_kernel(
    n_ep,
    n_tp,
    gated_ref,
    outw_ref,
    hid_ref,
    gain_ref,
    gate_ref,
    sel_ref,
    comb_hi_ref,
    comb_lo_ref,
    eg_hbm,
    eu_hbm,
    ed_hbm,
    dg_hbm,
    du_hbm,
    dd_hbm,
    mixed_ref,
    eg,
    eu,
    ed,
    dgw,
    duw,
    ddw,
    sel_recv,
    p_send,
    p_recv,
    st_send,
    st_recv,
    mid_buf,
    br_buf,
    piece,
    rows_all,
    g_send,
    g_recv,
    u_send,
    u_recv,
    e_hid,
    eo_send,
    eo_recv,
    d_hid,
    out_send,
    out_recv,
    ret_send,
    ret,
    w_sem,
    tp_ssem,
    tp_rsem,
    ep_ssem,
    ep_rsem,
):
    f32, bf16 = jnp.float32, jnp.bfloat16
    ep = lax.axis_index("ep")
    tp = lax.axis_index("tp")
    tokens, width = hid_ref.shape
    quarter = width // n_tp
    own = pl.ds(pl.multiple_of(tp * quarter, quarter), quarter)
    cap = sel_ref.shape[1]

    loads = []
    for i, (src, dst) in enumerate(
        ((dg_hbm, dgw), (du_hbm, duw), (eg_hbm, eg), (eu_hbm, eu), (ed_hbm, ed), (dd_hbm, ddw))
    ):
        load = pltpu.make_async_copy(src, dst, w_sem.at[i])
        load.start()
        loads.append(load)

    barrier = pltpu.get_barrier_semaphore()
    for d in range(1, n_tp):
        pl.semaphore_signal(
            barrier, inc=1, device_id=(ep, lax.rem(tp + d, n_tp)), device_id_type=MESH
        )
    for d in range(1, n_ep):
        pl.semaphore_signal(
            barrier, inc=1, device_id=(lax.rem(ep + d, n_ep), tp), device_id_type=MESH
        )

    def over_tp(phase, src_of, dst_of):
        copies = []
        for d in range(1, n_tp):
            peer = lax.rem(tp + d, n_tp)
            copy = pltpu.make_async_remote_copy(
                src_ref=src_of(peer),
                dst_ref=dst_of(d),
                send_sem=tp_ssem.at[phase, d - 1],
                recv_sem=tp_rsem.at[phase, d - 1],
                device_id=(ep, peer),
                device_id_type=MESH,
            )
            copy.start()
            copies.append(copy)
        return copies

    def over_ep(phase, src_of, dst_of):
        copies = []
        for d in range(1, n_ep):
            peer = lax.rem(ep + d, n_ep)
            copy = pltpu.make_async_remote_copy(
                src_ref=src_of(peer),
                dst_ref=dst_of(d),
                send_sem=ep_ssem.at[phase, d - 1],
                recv_sem=ep_rsem.at[phase, d - 1],
                device_id=(peer, tp),
                device_id_type=MESH,
            )
            copy.start()
            copies.append(copy)
        return copies

    def arrive(copies):
        for copy in copies:
            copy.wait_recv()

    for j in range(n_tp):
        p_send[j] = matmul(gated_ref[...], outw_ref[:, j * quarter : (j + 1) * quarter]).astype(bf16)
    pl.semaphore_wait(barrier, n_tp + n_ep - 2)
    c_part = over_tp(0, lambda peer: p_send.at[peer], lambda d: p_recv.at[d - 1])
    c_sel = over_ep(0, lambda peer: sel_ref.at[peer], lambda d: sel_recv.at[ep])
    sel_recv[ep] = sel_ref[ep]
    attended = p_send[tp].astype(f32)
    for d in range(1, n_tp):
        c_part[d - 1].wait_recv()
        attended = attended + p_recv[d - 1].astype(f32)
    middle = (hid_ref[:, own].astype(f32) + attended).astype(bf16).astype(f32)
    gain = gain_ref[:, own].astype(f32)
    squares = jnp.sum(middle * middle, axis=-1, keepdims=True)
    inner = jnp.sum(middle * gain * gate_ref[:, own].astype(f32), axis=-1, keepdims=True)
    lane = lax.broadcasted_iota(jnp.int32, (tokens, 128), 1)
    st_send[...] = jnp.where(lane < 64, squares, inner)
    c_stat = over_tp(1, lambda peer: st_send, lambda d: st_recv.at[d - 1])
    mid_buf[...] = middle
    totals = st_send[...]
    for d in range(1, n_tp):
        c_stat[d - 1].wait_recv()
        totals = totals + st_recv[d - 1]
    factor = lax.rsqrt(totals[:, 0:1] / width + EPSILON)
    br_buf[...] = jnp.broadcast_to(jax.nn.sigmoid(totals[:, 64:65] * factor), (tokens, 128))
    piece[ep] = (middle * factor * gain).astype(bf16)
    c_piece = over_ep(1, lambda peer: piece.at[ep], lambda d: piece.at[ep])

    arrive(c_sel)
    for d in range(n_ep):
        if d:
            c_piece[d - 1].wait_recv()
        source = lax.rem(ep - d + n_ep, n_ep)
        picked = matmul(sel_recv[source][:, :tokens], piece[source]).astype(bf16)
        rows_all[tp, pl.ds(pl.multiple_of(source * cap, cap), cap), :] = picked
    c_rows = over_tp(2, lambda peer: rows_all.at[tp], lambda d: rows_all.at[tp])

    loads[0].wait()
    loads[1].wait()
    everyone = piece[...].reshape(n_ep * tokens, quarter)
    units = dgw.shape[1]
    share = n_ep * tokens // n_tp
    g_send[...] = matmul(everyone, dgw[...]).astype(bf16).reshape(n_tp, share, units)
    c_g = over_tp(3, lambda peer: g_send.at[peer], lambda d: g_recv.at[d - 1])
    u_send[...] = matmul(everyone, duw[...]).astype(bf16).reshape(n_tp, share, units)
    c_u = over_tp(4, lambda peer: u_send.at[peer], lambda d: u_recv.at[d - 1])

    loads[2].wait()
    loads[3].wait()
    arrive(c_rows)
    block = eg.shape[1]
    tile = 256 if block % 256 == 0 else 128

    @pl.loop(0, block // tile)
    def _(i):
        cols = pl.ds(pl.multiple_of(i * tile, tile), tile)
        gate_part = matmul(rows_all[0], eg[0:quarter, cols])
        up_part = matmul(rows_all[0], eu[0:quarter, cols])
        for j in range(1, n_tp):
            span = slice(j * quarter, (j + 1) * quarter)
            gate_part = gate_part + matmul(rows_all[j], eg[span, cols])
            up_part = up_part + matmul(rows_all[j], eu[span, cols])
        e_hid[:, cols] = (silu(gate_part) * up_part).astype(bf16)

    g_sum = g_send[tp].astype(f32)
    u_sum = u_send[tp].astype(f32)
    for d in range(1, n_tp):
        c_g[d - 1].wait_recv()
        g_sum = g_sum + g_recv[d - 1].astype(f32)
    for d in range(1, n_tp):
        c_u[d - 1].wait_recv()
        u_sum = u_sum + u_recv[d - 1].astype(f32)
    d_hid[tp] = (silu(g_sum) * u_sum).astype(bf16)
    c_hid = over_tp(5, lambda peer: d_hid.at[tp], lambda d: d_hid.at[tp])

    loads[4].wait()
    for j in range(n_tp):
        eo_send[j] = matmul(e_hid[...], ed[:, j * quarter : (j + 1) * quarter]).astype(bf16)
    c_eo = over_tp(6, lambda peer: eo_send.at[peer], lambda d: eo_recv.at[d - 1])

    loads[5].wait()
    arrive(c_hid)
    hidden = d_hid[...].reshape(n_ep * tokens, units)
    out_send[...] = matmul(hidden, ddw[...]).astype(bf16).reshape(n_ep, tokens, quarter)
    c_out = over_ep(2, lambda peer: out_send.at[peer], lambda d: out_recv.at[d - 1])

    summed = eo_send[tp].astype(f32)
    for d in range(1, n_tp):
        c_eo[d - 1].wait_recv()
        summed = summed + eo_recv[d - 1].astype(f32)
    ret_send[...] = summed.astype(bf16).reshape(n_ep, cap, quarter)
    c_ret = over_ep(3, lambda peer: ret_send.at[peer], lambda d: ret.at[ep])
    ret[ep] = ret_send[ep]

    dense = out_send[ep].astype(f32)
    for d in range(1, n_ep):
        c_out[d - 1].wait_recv()
        dense = dense + out_recv[d - 1].astype(f32)
    arrive(c_ret)
    answers = ret[...].reshape(n_ep * cap, quarter)
    routed = matmul(comb_hi_ref[...], answers) + matmul(comb_lo_ref[...], answers)
    mixed_ref[...] = (mid_buf[...] + br_buf[:, 0:1] * dense + routed).astype(bf16)

    for copies in (c_part, c_sel, c_stat, c_piece, c_rows, c_g, c_u, c_hid, c_eo, c_out, c_ret):
        for copy in copies:
            copy.wait_send()


def run_layer(gated, output_weight, hid, gain, gate, sel, comb_hi, comb_lo, eg, eu, ed, dg, du, dd):
    n_ep, n_tp = lax.axis_size("ep"), lax.axis_size("tp")
    tokens = hid.shape[0]
    quarter = hid.shape[1] // n_tp
    cap = sel.shape[1]
    items = n_ep * cap
    share = n_ep * tokens // n_tp
    units = dg.shape[1]
    bf16, f32 = jnp.bfloat16, jnp.float32
    vmem = pl.BlockSpec(memory_space=pltpu.VMEM)
    anyspace = pl.BlockSpec(memory_space=pl.ANY)
    scratch = [pltpu.VMEM(w.shape, bf16) for w in (eg, eu, ed, dg, du, dd)]
    scratch += [
        pltpu.VMEM(sel.shape, bf16),
        pltpu.VMEM((n_tp, tokens, quarter), bf16),
        pltpu.VMEM((n_tp - 1, tokens, quarter), bf16),
        pltpu.VMEM((tokens, 128), f32),
        pltpu.VMEM((n_tp - 1, tokens, 128), f32),
        pltpu.VMEM((tokens, quarter), f32),
        pltpu.VMEM((tokens, 128), f32),
        pltpu.VMEM((n_ep, tokens, quarter), bf16),
        pltpu.VMEM((n_tp, items, quarter), bf16),
        pltpu.VMEM((n_tp, share, units), bf16),
        pltpu.VMEM((n_tp - 1, share, units), bf16),
        pltpu.VMEM((n_tp, share, units), bf16),
        pltpu.VMEM((n_tp - 1, share, units), bf16),
        pltpu.VMEM((items, eg.shape[1]), bf16),
        pltpu.VMEM((n_tp, items, quarter), bf16),
        pltpu.VMEM((n_tp - 1, items, quarter), bf16),
        pltpu.VMEM((n_tp, share, units), bf16),
        pltpu.VMEM((n_ep, tokens, quarter), bf16),
        pltpu.VMEM((n_ep - 1, tokens, quarter), bf16),
        pltpu.VMEM((n_ep, cap, quarter), bf16),
        pltpu.VMEM((n_ep, cap, quarter), bf16),
        pltpu.SemaphoreType.DMA((6,)),
        pltpu.SemaphoreType.DMA((7, n_tp - 1)),
        pltpu.SemaphoreType.DMA((7, n_tp - 1)),
        pltpu.SemaphoreType.DMA((4, n_ep - 1)),
        pltpu.SemaphoreType.DMA((4, n_ep - 1)),
    ]
    return pl.pallas_call(
        functools.partial(layer_kernel, n_ep, n_tp),
        out_shape=jax.ShapeDtypeStruct((tokens, quarter), bf16),
        in_specs=[vmem] * 8 + [anyspace] * 6,
        out_specs=vmem,
        scratch_shapes=scratch,
        compiler_params=pltpu.CompilerParams(
            collective_id=0, has_side_effects=True, vmem_limit_bytes=60 * 1024 * 1024
        ),
    )(gated, output_weight, hid, gain, gate, sel, comb_hi, comb_lo, eg, eu, ed, dg, du, dd)


def attention_kernel(
    cap,
    hidden_ref,
    gain_ref,
    shift_ref,
    head_gain_ref,
    routes_ref,
    weights_ref,
    qw_hbm,
    kw_hbm,
    vw_hbm,
    ow_hbm,
    fw_hbm,
    state_hbm,
    gated_ref,
    sel_ref,
    comb_hi_ref,
    comb_lo_ref,
    new_hbm,
    qw,
    kw,
    vw,
    ow,
    fw,
    state,
    query,
    key,
    value,
    decay,
    readout,
    w_sem,
    in_sem,
    out_sem,
):
    f32, bf16 = jnp.float32, jnp.bfloat16
    tokens = hidden_ref.shape[0]
    heads, key_dim, value_dim = state.shape[1:]
    groups = tokens // 8
    loads = []
    pairs = ((fw_hbm, fw), (kw_hbm, kw), (qw_hbm, qw), (vw_hbm, vw), (ow_hbm, ow))
    for i, (src, dst) in enumerate(pairs):
        load = pltpu.make_async_copy(src, dst, w_sem.at[i])
        load.start()
        loads.append(load)

    def fetch(g):
        rows = pl.ds(g * 8, 8)
        return pltpu.make_async_copy(state_hbm.at[rows], state.at[rows], in_sem.at[g])

    def put(g):
        rows = pl.ds(g * 8, 8)
        return pltpu.make_async_copy(state.at[rows], new_hbm.at[rows], out_sem.at[g])

    for g in range(groups):
        fetch(g).start()

    inputs = hidden_ref[...].astype(f32)
    normed = (inputs * rms_factor(inputs) * gain_ref[...].astype(f32)).astype(bf16)

    items = comb_hi_ref.shape[1]
    lane = lax.broadcasted_iota(jnp.int32, (tokens, 128), 1)
    first, second = routes_ref[:, 0:1], routes_ref[:, 1:2]
    chosen0 = jnp.where(lane == first, 1.0, 0.0)
    chosen1 = jnp.where(lane == second, 1.0, 0.0)
    row = lax.broadcasted_iota(jnp.int32, (tokens, tokens), 0)
    col = lax.broadcasted_iota(jnp.int32, (tokens, tokens), 1)
    before = jnp.where(row > col, 1.0, 0.0).astype(bf16)
    earlier = matmul(before, (chosen0 + chosen1).astype(bf16))
    slot0 = jnp.sum(earlier * chosen0, axis=1, keepdims=True)
    slot1 = jnp.sum(earlier * chosen1, axis=1, keepdims=True)
    table = lax.broadcasted_iota(jnp.int32, (tokens, items), 1)
    hit0 = table == first * cap + slot0.astype(jnp.int32)
    hit1 = table == second * cap + slot1.astype(jnp.int32)
    comb = jnp.where(hit0, weights_ref[:, 0:1], 0.0) + jnp.where(hit1, weights_ref[:, 1:2], 0.0)
    comb_hi = comb.astype(bf16)
    comb_hi_ref[...] = comb_hi
    comb_lo_ref[...] = (comb - comb_hi.astype(f32)).astype(bf16)
    onehot = (jnp.where(hit0, 1.0, 0.0) + jnp.where(hit1, 1.0, 0.0)).astype(bf16)
    lanes = sel_ref.shape[1]
    eye_row = lax.broadcasted_iota(jnp.int32, (tokens, lanes), 0)
    eye_col = lax.broadcasted_iota(jnp.int32, (tokens, lanes), 1)
    eye = jnp.where(eye_row == eye_col, 1.0, 0.0).astype(bf16)
    sel_ref[...] = lax.dot_general(
        onehot, eye, (((0,), (0,)), ((), ())), preferred_element_type=f32
    ).astype(bf16)

    def rounded_rows(weight):
        return matmul(normed, weight[...]).astype(bf16).astype(f32)

    loads[0].wait()
    drive = matmul(normed, fw[...])
    log_sig = jnp.minimum(drive, 0.0) - jnp.log1p(jnp.exp(-jnp.abs(drive)))
    decay[...] = jnp.exp(log_sig / TAU_DECAY + shift_ref[...]).reshape(decay.shape)
    loads[1].wait()
    key[...] = rounded_rows(kw).reshape(key.shape)
    loads[2].wait()
    query[...] = (rounded_rows(qw) * key_dim ** (-0.5)).reshape(query.shape)
    loads[3].wait()
    value[...] = rounded_rows(vw).reshape(value.shape)

    @pl.loop(0, groups)
    def _(g):
        fetch(g).wait()
        for h in range(heads):
            keys = slice(h * key_dim, (h + 1) * key_dim)
            vals = slice(h * value_dim, (h + 1) * value_dim)
            decay_cols = jnp.transpose(decay[g, :, keys])
            key_cols = jnp.transpose(key[g, :, keys])
            query_cols = jnp.transpose(query[g, :, keys])
            for j in range(8):
                fresh = (
                    decay_cols[:, j : j + 1] * state[g * 8 + j, h]
                    + key_cols[:, j : j + 1] * value[g, j : j + 1, vals]
                )
                state[g * 8 + j, h] = fresh
                readout[g, j : j + 1, vals] = jnp.sum(
                    query_cols[:, j : j + 1] * fresh, axis=0, keepdims=True
                )
        put(g).start()

    loads[4].wait()
    outgate = rounded_rows(ow)
    out = readout[...].reshape(tokens, heads * value_dim)
    for h in range(heads):
        vals = slice(h * value_dim, (h + 1) * value_dim)
        part = out[:, vals]
        gain = head_gain_ref[:, vals].astype(f32)
        gated_ref[:, vals] = (part * rms_factor(part) * gain * silu(outgate[:, vals])).astype(bf16)
    for g in range(groups):
        put(g).wait()


def run_attention(hidden, gain, shift, head_gain, routes, weights, qw, kw, vw, ow, fw, state, n_ep):
    bf16, f32 = jnp.bfloat16, jnp.float32
    tokens, heads, key_dim, value_dim = state.shape
    capacity = tokens * routes.shape[1] // n_ep + 2
    cap = (capacity + 15) // 16 * 16
    items = n_ep * cap
    groups = tokens // 8
    lanes = (tokens + 127) // 128 * 128
    vmem = pl.BlockSpec(memory_space=pltpu.VMEM)
    anyspace = pl.BlockSpec(memory_space=pl.ANY)
    gated, sel, comb_hi, comb_lo, new_state = pl.pallas_call(
        functools.partial(attention_kernel, cap),
        out_shape=(
            jax.ShapeDtypeStruct((tokens, heads * value_dim), bf16),
            jax.ShapeDtypeStruct((items, lanes), bf16),
            jax.ShapeDtypeStruct((tokens, items), bf16),
            jax.ShapeDtypeStruct((tokens, items), bf16),
            jax.ShapeDtypeStruct(state.shape, f32),
        ),
        in_specs=[vmem] * 6 + [anyspace] * 6,
        out_specs=(vmem, vmem, vmem, vmem, anyspace),
        scratch_shapes=[pltpu.VMEM(w.shape, bf16) for w in (qw, kw, vw, ow, fw)]
        + [
            pltpu.VMEM(state.shape, f32),
            pltpu.VMEM((groups, 8, heads * key_dim), f32),
            pltpu.VMEM((groups, 8, heads * key_dim), f32),
            pltpu.VMEM((groups, 8, heads * value_dim), f32),
            pltpu.VMEM((groups, 8, heads * key_dim), f32),
            pltpu.VMEM((groups, 8, heads * value_dim), f32),
            pltpu.SemaphoreType.DMA((5,)),
            pltpu.SemaphoreType.DMA((groups,)),
            pltpu.SemaphoreType.DMA((groups,)),
        ],
        compiler_params=pltpu.CompilerParams(vmem_limit_bytes=60 * 1024 * 1024),
    )(hidden, gain, shift, head_gain, routes, weights, qw, kw, vw, ow, fw, state)
    return gated, sel.reshape(n_ep, cap, lanes), comb_hi, comb_lo, new_state


def body(
    hidden_in,
    carried_state,
    input_gain,
    query_weight,
    key_weight,
    value_weight,
    outgate_weight,
    decay_weight,
    decay_shift,
    head_gain,
    output_weight,
    channel_gain,
    branch_gate,
    routes,
    route_weights,
    expert_gate,
    expert_up,
    expert_down,
    dense_gate,
    dense_up,
    dense_down,
):
    gated, sel, comb_hi, comb_lo, new_state = run_attention(
        hidden_in,
        input_gain[None, :],
        decay_shift,
        head_gain.reshape(1, -1),
        routes,
        route_weights,
        query_weight,
        key_weight,
        value_weight,
        outgate_weight,
        decay_weight,
        carried_state,
        lax.axis_size("ep"),
    )
    mixed = run_layer(
        gated,
        output_weight,
        hidden_in,
        channel_gain[None, :],
        branch_gate[None, :],
        sel,
        comb_hi,
        comb_lo,
        expert_gate[0],
        expert_up[0],
        expert_down[0],
        dense_gate,
        dense_up,
        dense_down,
    )
    return (mixed, new_state)


def solution(mesh):
    in_specs = (
        P("ep", None),
        P("ep", "tp", None, None),
        P(),
        P(None, "tp"),
        P(None, "tp"),
        P(None, "tp"),
        P(None, "tp"),
        P(None, "tp"),
        P("ep", "tp"),
        P("tp", None),
        P("tp", None),
        P(),
        P(),
        P("ep", None),
        P("ep", None),
        P("ep", None, "tp"),
        P("ep", None, "tp"),
        P("ep", "tp", None),
        P("tp", "ep"),
        P("tp", "ep"),
        P("ep", "tp"),
    )
    out_specs = (P("ep", "tp"), P("ep", "tp", None, None))
    return jax.shard_map(body, mesh=mesh, in_specs=in_specs, out_specs=out_specs, check_vma=False)
```
